512 devices in a mesh: sp: 16 (over z), dp: 32 (over y, x, core).
Axes of the slice: x: 4, y: 4, z: 16, core: 2. Of those that a mesh axis runs over, the one named last changes fastest.
Arguments:
- queries: bfloat16 [32, 2048, 1024], P('dp', 'sp'), may hold values from -6 to 6
- key_rows: bfloat16 [32, 2048, 1024], P('dp', 'sp'), may hold values from -6 to 6
- value_rows: bfloat16 [32, 2048, 1024], P('dp', 'sp'), may hold values from -6 to 6
- break_offset: bfloat16 [32, 2048, 16], P('dp', 'sp'), may hold values from 1.5 to 15
- hidden_in: bfloat16 [32, 2048, 2048], P('dp', 'sp'), may hold values from -6 to 6
- gate_weight: bfloat16 [2048, 1024], P('dp', 'sp'), may hold values from -0.125 to 0.125
- out_weight: bfloat16 [1024, 2048], P('sp', 'dp'), may hold values from -0.1875 to 0.1875
Outputs:
- mixed: bfloat16 [32, 2048, 2048], P('dp', 'sp')
The draws below stay inside these ranges and needn't reach their ends.
All inputs are finite; a program needn't handle non-finite values.
Results may differ from the reference program's by a relative error of at most 0.0063.
Values may be sent and summed in bfloat16 or wider, within the bound.
No kernel may reach another device: no remote copies, remote signals or barrier semaphores. Data moves between devices by JAX's collectives and lax.ppermute only.
A program may use at most 64 MiB of HBM per device.

```python
import math
import jax
import jax.numpy as jnp
from jax import lax

D = 2048
HEADS = 16
HD = 64
HH = 1024
BATCH = 32
LENGTH = 2048


def draw_break_offset(key, part):
    head_key, base_key, span_key, rough_key = jax.random.split(jax.random.fold_in(key, 17), 4)
    fast_share = 0.5
    fast_heads = jax.random.uniform(head_key, (HEADS,)) < fast_share
    spread = jax.random.uniform(base_key, (HEADS,))
    base = jnp.where(fast_heads, 3.0 + spread, math.log(LENGTH) + 1.0 + spread)
    spans = jax.random.uniform(span_key, (BATCH, LENGTH // 64, HEADS), minval=-0.7, maxval=0.7)
    spans = jnp.repeat(spans, 64, axis=1)
    rough = jax.random.uniform(rough_key, (BATCH, LENGTH, HEADS), minval=-0.5, maxval=0.5)
    return (base[None, None, :] + spans + rough).astype(jnp.bfloat16)


def block_levels(stream_key, shape, cuts, smallest, high):
    gain, own = 1.0, jax.random.fold_in(stream_key, 6)
    for dim, parts in cuts:
        heights = jnp.exp(jax.random.uniform(jax.random.fold_in(own, dim), (parts,), jnp.float32, smallest / len(cuts), high / len(cuts)))
        gain = gain * jnp.repeat(heights, shape[dim] // parts).reshape([-1 if axis == dim else 1 for axis in range(len(shape))])
    return gain


def bell_draw(rng, dims, scale, bound, cuts=(), kind=jnp.bfloat16):
    entries = jax.random.normal(rng, dims, jnp.float32) * scale
    if len(cuts) > 0:
        entries = block_levels(rng, dims, cuts, -0.22, 0.18) * entries
    return jnp.clip(entries, min=-bound, max=bound).astype(kind)


def setup_inputs(seed: int = 0) -> dict:
    streams_of = jax.random.split(jax.random.key(seed), 8)
    return {
        "queries": bell_draw(streams_of[0], (BATCH, LENGTH, HH), 1.0, 6.0, ((0, 32), (1, 16))),
        "key_rows": bell_draw(streams_of[1], (BATCH, LENGTH, HH), 1.0, 6.0, ((0, 32), (1, 16))),
        "value_rows": bell_draw(streams_of[2], (BATCH, LENGTH, HH), 1.0, 6.0, ((0, 32), (1, 16))),
        "break_offset": draw_break_offset(jax.random.fold_in(streams_of[7], 71), 0),
        "hidden_in": bell_draw(streams_of[4], (BATCH, LENGTH, D), 1.0, 6.0, ((0, 32), (1, 16))),
        "gate_weight": bell_draw(streams_of[5], (D, HH), D ** -0.5, 0.125, ((0, 32), (1, 16))),
        "out_weight": bell_draw(streams_of[6], (HH, D), HH ** -0.5, 0.1875, ((0, 16), (1, 32))),
    }


eps_norm = 1e-05

def stick_heads(queries, key_rows, value_rows, offsets):
    block_rows = min(512, LENGTH)
    score_scale = HD ** (-0.5)
    key_pos = jnp.arange(LENGTH).astype(jnp.int32)

    def one_block(block_index):
        first_row = (block_index * block_rows).astype(jnp.int32)
        query_block = lax.dynamic_slice_in_dim(queries, first_row, block_rows, 1)
        scores = jnp.einsum('hqd,hkd->hqk', query_block, key_rows) * score_scale - offsets[:, None, :]
        query_pos = first_row + jnp.arange(block_rows).astype(jnp.int32)
        earlier = key_pos[None, :] < query_pos[:, None]
        keep_log = jnp.where(earlier, jax.nn.log_sigmoid(-scores), 0.0)
        later_sum = lax.cumsum(keep_log, axis=2, reverse=True) - keep_log
        weights = jnp.where(earlier, jnp.exp(jax.nn.log_sigmoid(scores) + later_sum), 0.0).astype(jnp.bfloat16)
        return jnp.einsum('hqk,hkd->hqd', weights.astype(jnp.float32), value_rows)
    blocks = lax.map(one_block, jnp.arange(LENGTH // block_rows).astype(jnp.int32))
    return blocks.transpose(1, 0, 2, 3).reshape(HEADS, LENGTH, HD)

def reference(queries, key_rows, value_rows, break_offset, hidden_in, gate_weight, out_weight):

    def heads_first(array):
        return array.astype(jnp.float32).reshape(LENGTH, HEADS, HD).transpose(1, 0, 2)

    def one_sequence(inputs):
        seq_queries, seq_keys, seq_values, seq_offsets, seq_hidden = inputs
        heads_out = stick_heads(heads_first(seq_queries), heads_first(seq_keys), heads_first(seq_values), seq_offsets.astype(jnp.float32).T)
        mean_sq = lax.optimization_barrier(jnp.mean(heads_out * heads_out, axis=2, keepdims=True))
        normed = (heads_out * lax.rsqrt(mean_sq + eps_norm)).astype(jnp.bfloat16)
        normed = normed.transpose(1, 0, 2).reshape(LENGTH, HH)
        gate_act = jax.nn.silu(jnp.dot(seq_hidden, gate_weight, preferred_element_type=jnp.float32))
        gated = (normed.astype(jnp.float32) * gate_act).astype(jnp.bfloat16)
        return jnp.dot(gated, out_weight, preferred_element_type=jnp.float32).astype(jnp.bfloat16)
    return lax.map(one_sequence, (queries, key_rows, value_rows, break_offset, hidden_in))
```

```python
import math
import jax
import jax.numpy as jnp
from jax import lax
from jax.experimental import pallas as pl
from jax.experimental.pallas import tpu as pltpu
from jax.sharding import PartitionSpec as P

eps_norm = 1e-05
log2e = math.log2(math.e)
score_cap = 25.0
f32, bf16 = jnp.float32, jnp.bfloat16
SRC, TOK, HD, GRP = 16, 128, 64, 4
ROWS = TOK + TOK // 2 + 8


def mm(a, b, ca=1, cb=0):
    return lax.dot_general(a, b, (((ca,), (cb,)), ((), ())), preferred_element_type=f32)


def pack_kernel(q_ref, k_ref, v_ref, o_ref, out_ref):
    row = lax.broadcasted_iota(jnp.int32, (TOK, TOK), 0)
    col = lax.broadcasted_iota(jnp.int32, (TOK, TOK), 1)
    perm = jnp.where(col == GRP * (row % 32) + row // 32, 1.0, 0.0).astype(bf16)
    keys = mm(perm, k_ref[0]).astype(bf16)
    vals = mm(perm, v_ref[0]).astype(bf16)
    offs = mm(o_ref[0], perm, 0, 1).astype(bf16)
    for h in range(SRC):
        s = slice(HD * h, HD * h + HD)
        out_ref[h, 0:TOK, :] = jnp.concatenate([q_ref[0, :, s], keys[:, s]], axis=1)
        out_ref[h, TOK:192, :] = jnp.concatenate([vals[0:64, s], vals[64:128, s]], axis=1)
        out_ref[h, 192:200, :] = jnp.broadcast_to(offs[h : h + 1, :], (8, TOK))


def pack(q, k, v, o):
    return pl.pallas_call(
        pack_kernel,
        out_shape=jax.ShapeDtypeStruct((SRC, ROWS, TOK), bf16),
    )(q, k, v, o)


def attn_kernel(buf_ref, out_ref, qq, kk, vv, of):
    nblk = SRC // GRP
    for i in range(SRC):
        q = buf_ref[i, 0:TOK, 0:HD].astype(f32) * (log2e / 8.0)
        hi = q.astype(bf16)
        lo = (q - hi.astype(f32)).astype(bf16)
        qq[TOK * i : TOK * i + TOK, :] = jnp.concatenate([hi, lo], axis=1)
        for g in range(GRP):
            k = buf_ref[i, 32 * g : 32 * g + 32, HD : 2 * HD]
            r = 512 * (i // 4) + 128 * g + 32 * (i % 4)
            kk[r : r + 32, :] = jnp.concatenate([k, k], axis=1)
            vr = TOK + 32 * (g % 2)
            vv[r : r + 32, :] = buf_ref[i, vr : vr + 32, HD * (g // 2) : HD * (g // 2) + HD]
    lane1 = lax.broadcasted_iota(jnp.int32, (8, TOK), 1)
    for b in range(nblk):
        rows = [buf_ref[4 * b + i, 192:200, :].astype(f32) * log2e for i in range(4)]
        for g in range(GRP):
            parts = [r if (i == g) else pltpu.roll(r, (32 * (i - g)) % TOK, 1) for i, r in enumerate(rows)]
            o = parts[3]
            for i in range(3):
                o = jnp.where(lane1 // 32 == i, parts[i], o)
            of[8 * (GRP * b + g) : 8 * (GRP * b + g) + 8, :] = o
    tr = lax.broadcasted_iota(jnp.int32, (256, 256), 0) % TOK
    tc = lax.broadcasted_iota(jnp.int32, (256, 256), 1)
    tri = jnp.where((tc >= TOK) | (tr > tc), -1.0, 0.0).astype(bf16)

    R = 256

    def block(qt, b, qrow, carry, acc, diag):
        ks = b * 512
        if not isinstance(b, int):
            ks = pl.multiple_of(ks, 512)
        x = mm(qt, kk[pl.ds(ks, 512), :], 1, 1)
        e, a = [], []
        for g in range(GRP):
            ob = b * 32 + 8 * g
            if not isinstance(b, int):
                ob = pl.multiple_of(ob, 8)
            off = of[pl.ds(ob, 8), :][0:1, :]
            eg = jnp.exp2(jnp.minimum(x[:, 128 * g : 128 * g + 128] - off, score_cap))
            if diag:
                m = lax.broadcasted_iota(jnp.int32, (R, TOK), 1)
                t = lax.broadcasted_iota(jnp.int32, (R, TOK), 0)
                eg = jnp.where(GRP * m + g < t + qrow, eg, 0.0)
            e.append(eg)
            a.append(1.0 + eg)
        lg = jnp.log2((a[0] * a[1]) * (a[2] * a[3]))
        hi = lg.astype(bf16)
        lo = (lg - hi.astype(f32)).astype(bf16)
        cc = mm(jnp.concatenate([hi, lo], axis=1), tri)
        t = jnp.exp2((cc[:, 0:TOK] + carry) - lg)
        carry = carry + cc[:, TOK:]
        w0 = e[0] * t
        t = t * a[0]
        w1 = e[1] * t
        t = t * a[1]
        w2 = e[2] * t
        t = t * a[2]
        w3 = e[3] * t
        w = jnp.concatenate([u.astype(bf16) for u in (w0, w1, w2, w3)], axis=1)
        acc = acc + mm(w, vv[pl.ds(ks, 512), :])
        return carry, acc

    for j in range(2048 // R):
        qt = qq[R * j : R * j + R, :]
        carry = jnp.zeros((R, TOK), f32)
        acc = jnp.zeros((R, HD), f32)
        db = (R * j) // 512
        carry, acc = block(qt, db, R * j - 512 * db, carry, acc, True)
        for b in range(db - 1, -1, -1):
            carry, acc = block(qt, b, 0, carry, acc, False)
        n = acc * lax.rsqrt(jnp.mean(acc * acc, axis=1, keepdims=True) + eps_norm)
        n = n.astype(bf16)
        for d in range(R // TOK):
            lo_, hi_ = n[TOK * d : TOK * d + 64], n[TOK * d + 64 : TOK * d + TOK]
            out_ref[(R // TOK) * j + d] = jnp.concatenate([lo_, hi_], axis=1)


def attend(buf):
    return pl.pallas_call(
        attn_kernel,
        out_shape=jax.ShapeDtypeStruct((SRC, 64, TOK), bf16),
        scratch_shapes=[
            pltpu.VMEM((2048, 128), bf16),
            pltpu.VMEM((2048, 128), bf16),
            pltpu.VMEM((2048, HD), bf16),
            pltpu.VMEM((128, TOK), f32),
        ],
        compiler_params=pltpu.CompilerParams(vmem_limit_bytes=48 * 1024 * 1024),
    )(buf)


def gate_kernel(h_ref, w_ref, out_ref, acc_ref):
    j = pl.program_id(0)
    w = w_ref[:, 0].reshape(256, 1024)
    part = mm(h_ref[0], w)

    @pl.when(j == 0)
    def _():
        acc_ref[...] = part

    @pl.when(j > 0)
    def _():
        acc_ref[...] += part

    @pl.when(j == pl.num_programs(0) - 1)
    def _():
        v = acc_ref[...]
        out_ref[...] = v / (1.0 + jnp.exp(-v))


def gate(hidden, w):
    return pl.pallas_call(
        gate_kernel,
        grid=(8,),
        in_specs=[
            pl.BlockSpec((1, TOK, 256), lambda j: (0, 0, j)),
            pl.BlockSpec((4, 1, 64, 1024), lambda j: (j, 0, 0, 0)),
        ],
        out_specs=pl.BlockSpec((TOK, 1024), lambda j: (0, 0)),
        out_shape=jax.ShapeDtypeStruct((TOK, 1024), f32),
        scratch_shapes=[pltpu.VMEM((TOK, 1024), f32)],
        cost_estimate=pl.CostEstimate(flops=2 * 128 * 1024 * 2048, bytes_accessed=5 << 20, transcendentals=1 << 17),
    )(hidden, w)


def mix_kernel(r_ref, g_ref, w_ref, out_ref, gd_ref):
    @pl.when(pl.program_id(0) == 0)
    def _():
        for h in range(0, SRC, 2):
            a, b = r_ref[h], r_ref[h + 1]
            top = jnp.concatenate([a[:, 0:HD], b[:, 0:HD]], axis=1)
            bot = jnp.concatenate([a[:, HD:], b[:, HD:]], axis=1)
            n = jnp.concatenate([top, bot], axis=0).astype(f32)
            s = slice(HD * h, HD * h + 2 * HD)
            gd_ref[:, s] = (n * g_ref[:, s]).astype(bf16)

    w = w_ref[:, 0].reshape(256, 1024)
    out_ref[0] = mm(gd_ref[...], w, 1, 1).astype(bf16)


def mix(ret, gact, w):
    return pl.pallas_call(
        mix_kernel,
        grid=(8,),
        in_specs=[
            pl.BlockSpec((SRC, 64, TOK), lambda j: (0, 0, 0)),
            pl.BlockSpec((TOK, 1024), lambda j: (0, 0)),
            pl.BlockSpec((4, 1, 64, 1024), lambda j: (j, 1, 0, 0)),
        ],
        out_specs=pl.BlockSpec((1, TOK, 256), lambda j: (0, 0, j)),
        out_shape=jax.ShapeDtypeStruct((1, TOK, 2048), bf16),
        scratch_shapes=[pltpu.VMEM((TOK, 1024), bf16)],
        cost_estimate=pl.CostEstimate(flops=2 * 128 * 1024 * 2048, bytes_accessed=6 << 20, transcendentals=0),
    )(ret, gact, w)


def turn_kernel(x_ref, out_ref):
    out_ref[...] = x_ref[...].T


def turn(x):
    return pl.pallas_call(turn_kernel, out_shape=jax.ShapeDtypeStruct((128, 1024), bf16))(x)


def shards(queries, key_rows, value_rows, break_offset, hidden_in, gate_weight, out_weight):
    own = jnp.concatenate([gate_weight.T, out_weight], axis=1)
    cols = turn(lax.all_gather(own, "sp", axis=0, tiled=True))
    w = lax.all_gather(cols[None], "dp", axis=0, tiled=True).reshape(32, 2, 64, 1024)
    buf = pack(queries, key_rows, value_rows, break_offset)
    buf = lax.all_to_all(buf, "sp", split_axis=0, concat_axis=0, tiled=True)
    heads = attend(buf)
    ret = lax.all_to_all(heads, "sp", split_axis=0, concat_axis=0, tiled=True)
    return mix(ret, gate(hidden_in, w), w)


def solution(mesh):
    tok = P("dp", "sp", None)
    return jax.shard_map(
        shards,
        mesh=mesh,
        in_specs=(tok, tok, tok, tok, tok, P("dp", "sp"), P("sp", "dp")),
        out_specs=tok,
        check_vma=False,
    )
```

```python
import math
import jax
import jax.numpy as jnp
from jax import lax
from jax.experimental import pallas as pl
from jax.experimental.pallas import tpu as pltpu
from jax.sharding import PartitionSpec as P


eps_norm = 1e-05
log2e = math.log2(math.e)
score_cap = 25.0
f32, bf16 = jnp.float32, jnp.bfloat16
SRC, TOK, HD, GRP = 16, 128, 64, 4
ROWS = TOK + TOK // 2 + 8


def mm(a, b, ca=1, cb=0):
    return lax.dot_general(a, b, (((ca,), (cb,)), ((), ())), preferred_element_type=f32)


def pack_kernel(q_ref, k_ref, v_ref, o_ref, out_ref):
    row = lax.broadcasted_iota(jnp.int32, (TOK, TOK), 0)
    col = lax.broadcasted_iota(jnp.int32, (TOK, TOK), 1)
    perm = jnp.where(col == GRP * (row % 32) + row // 32, 1.0, 0.0).astype(bf16)
    keys = mm(perm, k_ref[0]).astype(bf16)
    vals = mm(perm, v_ref[0]).astype(bf16)
    offs = mm(o_ref[0], perm, 0, 1).astype(bf16)
    for h in range(SRC):
        s = slice(HD * h, HD * h + HD)
        out_ref[h, 0:TOK, :] = jnp.concatenate([q_ref[0, :, s], keys[:, s]], axis=1)
        out_ref[h, TOK:192, :] = jnp.concatenate([vals[0:64, s], vals[64:128, s]], axis=1)
        out_ref[h, 192:200, :] = jnp.broadcast_to(offs[h : h + 1, :], (8, TOK))


def pack(q, k, v, o):
    return pl.pallas_call(
        pack_kernel,
        out_shape=jax.ShapeDtypeStruct((SRC, ROWS, TOK), bf16),
    )(q, k, v, o)


def attn_kernel(buf_ref, out_ref, qq, kk, vv, of):
    nblk = SRC // GRP
    for i in range(SRC):
        q = buf_ref[i, 0:TOK, 0:HD].astype(f32) * (log2e / 8.0)
        hi = q.astype(bf16)
        lo = (q - hi.astype(f32)).astype(bf16)
        qq[TOK * i : TOK * i + TOK, :] = jnp.concatenate([hi, lo], axis=1)
        for g in range(GRP):
            k = buf_ref[i, 32 * g : 32 * g + 32, HD : 2 * HD]
            r = 512 * (i // 4) + 128 * g + 32 * (i % 4)
            kk[r : r + 32, :] = jnp.concatenate([k, k], axis=1)
            vr = TOK + 32 * (g % 2)
            vv[r : r + 32, :] = buf_ref[i, vr : vr + 32, HD * (g // 2) : HD * (g // 2) + HD]
    lane1 = lax.broadcasted_iota(jnp.int32, (8, TOK), 1)
    for b in range(nblk):
        rows = [buf_ref[4 * b + i, 192:200, :].astype(f32) * log2e for i in range(4)]
        for g in range(GRP):
            parts = [r if (i == g) else pltpu.roll(r, (32 * (i - g)) % TOK, 1) for i, r in enumerate(rows)]
            o = parts[3]
            for i in range(3):
                o = jnp.where(lane1 // 32 == i, parts[i], o)
            of[8 * (GRP * b + g) : 8 * (GRP * b + g) + 8, :] = o
    tr = lax.broadcasted_iota(jnp.int32, (256, 256), 0) % TOK
    tc = lax.broadcasted_iota(jnp.int32, (256, 256), 1)
    tri = jnp.where((tc >= TOK) | (tr > tc), -1.0, 0.0).astype(bf16)

    R = 256

    def block(qt, b, qrow, carry, acc, diag):
        ks = b * 512
        if not isinstance(b, int):
            ks = pl.multiple_of(ks, 512)
        x = mm(qt, kk[pl.ds(ks, 512), :], 1, 1)
        e, a = [], []
        for g in range(GRP):
            ob = b * 32 + 8 * g
            if not isinstance(b, int):
                ob = pl.multiple_of(ob, 8)
            off = of[pl.ds(ob, 8), :][0:1, :]
            eg = jnp.exp2(jnp.minimum(x[:, 128 * g : 128 * g + 128] - off, score_cap))
            if diag:
                m = lax.broadcasted_iota(jnp.int32, (R, TOK), 1)
                t = lax.broadcasted_iota(jnp.int32, (R, TOK), 0)
                eg = jnp.where(GRP * m + g < t + qrow, eg, 0.0)
            e.append(eg)
            a.append(1.0 + eg)
        lg = jnp.log2((a[0] * a[1]) * (a[2] * a[3]))
        hi = lg.astype(bf16)
        lo = (lg - hi.astype(f32)).astype(bf16)
        cc = mm(jnp.concatenate([hi, lo], axis=1), tri)
        t = jnp.exp2((cc[:, 0:TOK] + carry) - lg)
        carry = carry + cc[:, TOK:]
        w0 = e[0] * t
        t = t * a[0]
        w1 = e[1] * t
        t = t * a[1]
        w2 = e[2] * t
        t = t * a[2]
        w3 = e[3] * t
        w = jnp.concatenate([u.astype(bf16) for u in (w0, w1, w2, w3)], axis=1)
        acc = acc + mm(w, vv[pl.ds(ks, 512), :])
        return carry, acc

    for j in range(2048 // R):
        qt = qq[R * j : R * j + R, :]
        carry = jnp.zeros((R, TOK), f32)
        acc = jnp.zeros((R, HD), f32)
        db = (R * j) // 512
        carry, acc = block(qt, db, R * j - 512 * db, carry, acc, True)
        for b in range(db - 1, -1, -1):
            carry, acc = block(qt, b, 0, carry, acc, False)
        n = acc * lax.rsqrt(jnp.mean(acc * acc, axis=1, keepdims=True) + eps_norm)
        n = n.astype(bf16)
        for d in range(R // TOK):
            lo_, hi_ = n[TOK * d : TOK * d + 64], n[TOK * d + 64 : TOK * d + TOK]
            out_ref[(R // TOK) * j + d] = jnp.concatenate([lo_, hi_], axis=1)


def attend(buf):
    return pl.pallas_call(
        attn_kernel,
        out_shape=jax.ShapeDtypeStruct((SRC, 64, TOK), bf16),
        scratch_shapes=[
            pltpu.VMEM((2048, 128), bf16),
            pltpu.VMEM((2048, 128), bf16),
            pltpu.VMEM((2048, HD), bf16),
            pltpu.VMEM((128, TOK), f32),
        ],
        compiler_params=pltpu.CompilerParams(vmem_limit_bytes=48 * 1024 * 1024),
    )(buf)


def turn_kernel(x_ref, out_ref):
    out_ref[...] = x_ref[...].T


def turn(x):
    return pl.pallas_call(turn_kernel, out_shape=jax.ShapeDtypeStruct((128, 1024), bf16))(x)


def two_chips(pos_ref, own_ref, sib_ref, j):
    p = pos_ref[0]
    south, x, y = (p & 1) == 0, (p >> 1) & 3, p >> 3
    rows = []
    for chip in (2 * j, 2 * j + 1):
        dy, dx = (y - chip // 4) & 3, (x - chip % 4) & 3
        first, second = 4 * dy + dx, 4 * dx + dy
        a = own_ref[jnp.where(south, first, second)]
        b = sib_ref[jnp.where(south, second, first)]
        rows += [jnp.where(south, a, b), jnp.where(south, b, a)]
    return jnp.concatenate(rows, axis=0)


def gate_kernel(pos_ref, h_ref, own_ref, sib_ref, out_ref):
    acc = jnp.zeros((TOK, 1024), f32)
    for j in range(8):
        acc = acc + mm(h_ref[0, :, 256 * j : 256 * j + 256], two_chips(pos_ref, own_ref, sib_ref, j))
    out_ref[...] = acc / (1.0 + jnp.exp(-acc))


def mix_kernel(pos_ref, r_ref, g_ref, own_ref, sib_ref, out_ref, gd_ref):
    for h in range(0, SRC, 2):
        a, b = r_ref[h], r_ref[h + 1]
        top = jnp.concatenate([a[:, 0:HD], b[:, 0:HD]], axis=1)
        bot = jnp.concatenate([a[:, HD:], b[:, HD:]], axis=1)
        n = jnp.concatenate([top, bot], axis=0).astype(f32)
        s = slice(HD * h, HD * h + 2 * HD)
        gd_ref[:, s] = (n * g_ref[:, s]).astype(bf16)
    for j in range(8):
        w = two_chips(pos_ref, own_ref, sib_ref, j)
        out_ref[0, :, 256 * j : 256 * j + 256] = mm(gd_ref[...], w, 1, 1).astype(bf16)


def whole(n, smem=1):
    spec = [pl.BlockSpec(memory_space=pltpu.SMEM)] * smem
    return spec + [pl.BlockSpec(memory_space=pltpu.VMEM)] * n


def gate(tab, hidden, own, sib):
    return pl.pallas_call(
        gate_kernel,
        in_specs=whole(3),
        out_shape=jax.ShapeDtypeStruct((TOK, 1024), f32),
        compiler_params=pltpu.CompilerParams(vmem_limit_bytes=40 * 1024 * 1024),
        cost_estimate=pl.CostEstimate(flops=2 * 128 * 1024 * 2048, bytes_accessed=5 << 20, transcendentals=1 << 17),
    )(tab, hidden, own, sib)


def mix(tab, ret, gact, own, sib):
    return pl.pallas_call(
        mix_kernel,
        in_specs=whole(4),
        out_shape=jax.ShapeDtypeStruct((1, TOK, 2048), bf16),
        scratch_shapes=[pltpu.VMEM((TOK, 1024), bf16)],
        compiler_params=pltpu.CompilerParams(vmem_limit_bytes=40 * 1024 * 1024),
        cost_estimate=pl.CostEstimate(flops=2 * 128 * 1024 * 2048, bytes_accessed=6 << 20, transcendentals=0),
    )(tab, ret, gact, own, sib)


def moves(phase, step):
    out = []
    for y in range(4):
        for x in range(4):
            for c in range(2):
                along_x = (c == 0) == (phase == 1)
                ty, tx = (y, (x + step) % 4) if along_x else ((y + step) % 4, x)
                out.append(((y * 4 + x) * 2 + c, (ty * 4 + tx) * 2 + c))
    return out


def ring(b, phase):
    back1 = lax.ppermute(b, "dp", moves(phase, 1))
    back3 = lax.ppermute(b, "dp", moves(phase, -1))
    top = lax.ppermute(b[..., :64, :], "dp", moves(phase, 2))
    bot = lax.ppermute(b[..., 64:, :], "dp", moves(phase, -2))
    return back1, back3, top, bot


def shards(queries, key_rows, value_rows, break_offset, hidden_in, gate_weight, out_weight):
    buf = pack(queries, key_rows, value_rows, break_offset)
    joined = jnp.concatenate([gate_weight.T, out_weight], axis=1)
    buf, joined = lax.optimization_barrier((buf, joined))
    joined = lax.all_gather(joined, "sp", axis=0, tiled=True)
    buf, joined = lax.optimization_barrier((buf, joined))
    buf = lax.all_to_all(buf, "sp", split_axis=0, concat_axis=0, tiled=True)
    b = turn(joined)
    back1, back3, top, bot = ring(b, 1)
    b = jnp.stack([b, back1, jnp.concatenate([top, bot], axis=0), back3])
    back1, back3, top, bot = ring(b, 2)
    own_g = jnp.concatenate([b[:, :64], back1[:, :64], top, back3[:, :64]], axis=0)
    own_o = jnp.concatenate([b[:, 64:], back1[:, 64:], bot, back3[:, 64:]], axis=0)
    swap = [(p, p ^ 1) for p in range(32)]
    sib_g = lax.ppermute(own_g, "dp", swap)
    sib_o = lax.ppermute(own_o, "dp", swap)
    pos = lax.axis_index("dp").astype(jnp.int32).reshape(1)
    heads = attend(buf)
    ret = lax.all_to_all(heads, "sp", split_axis=0, concat_axis=0, tiled=True)
    gact = gate(pos, hidden_in, own_g, sib_g)
    return mix(pos, ret, gact, own_o, sib_o)


def solution(mesh):
    tok = P("dp", "sp", None)
    return jax.shard_map(
        shards,
        mesh=mesh,
        in_specs=(tok, tok, tok, tok, tok, P("dp", "sp"), P("sp", "dp")),
        out_specs=tok,
        check_vma=False,
    )
```

```python
import math
import jax
import jax.numpy as jnp
from jax import lax
from jax.experimental import pallas as pl
from jax.experimental.pallas import tpu as pltpu
from jax.sharding import PartitionSpec as P


eps_norm = 1e-05
log2e = math.log2(math.e)
score_cap = 25.0
f32, bf16 = jnp.float32, jnp.bfloat16
SRC, TOK, HD, GRP = 16, 128, 64, 4
ROWS = TOK + TOK // 2 + 8


def mm(a, b, ca=1, cb=0):
    return lax.dot_general(a, b, (((ca,), (cb,)), ((), ())), preferred_element_type=f32)


def pack_kernel(q_ref, k_ref, v_ref, o_ref, out_ref):
    row = lax.broadcasted_iota(jnp.int32, (TOK, TOK), 0)
    col = lax.broadcasted_iota(jnp.int32, (TOK, TOK), 1)
    perm = jnp.where(col == GRP * (row % 32) + row // 32, 1.0, 0.0).astype(bf16)
    keys = mm(perm, k_ref[0]).astype(bf16)
    vals = mm(perm, v_ref[0]).astype(bf16)
    offs = mm(o_ref[0], perm, 0, 1).astype(bf16)
    for h in range(SRC):
        s = slice(HD * h, HD * h + HD)
        out_ref[h, 0:TOK, :] = jnp.concatenate([q_ref[0, :, s], keys[:, s]], axis=1)
        out_ref[h, TOK:192, :] = jnp.concatenate([vals[0:64, s], vals[64:128, s]], axis=1)
        out_ref[h, 192:200, :] = jnp.broadcast_to(offs[h : h + 1, :], (8, TOK))


def pack(q, k, v, o):
    return pl.pallas_call(
        pack_kernel,
        out_shape=jax.ShapeDtypeStruct((SRC, ROWS, TOK), bf16),
    )(q, k, v, o)


def attn_kernel(buf_ref, out_ref, qq, kk, vv, of):
    nblk = SRC // GRP
    for i in range(SRC):
        q = buf_ref[i, 0:TOK, 0:HD].astype(f32) * (log2e / 8.0)
        hi = q.astype(bf16)
        lo = (q - hi.astype(f32)).astype(bf16)
        qq[TOK * i : TOK * i + TOK, :] = jnp.concatenate([hi, lo], axis=1)
        for g in range(GRP):
            k = buf_ref[i, 32 * g : 32 * g + 32, HD : 2 * HD]
            r = 512 * (i // 4) + 128 * g + 32 * (i % 4)
            kk[r : r + 32, :] = jnp.concatenate([k, k], axis=1)
            vr = TOK + 32 * (g % 2)
            vv[r : r + 32, :] = buf_ref[i, vr : vr + 32, HD * (g // 2) : HD * (g // 2) + HD]
    lane1 = lax.broadcasted_iota(jnp.int32, (8, TOK), 1)
    for b in range(nblk):
        rows = [buf_ref[4 * b + i, 192:200, :].astype(f32) * log2e for i in range(4)]
        for g in range(GRP):
            parts = [r if (i == g) else pltpu.roll(r, (32 * (i - g)) % TOK, 1) for i, r in enumerate(rows)]
            o = parts[3]
            for i in range(3):
                o = jnp.where(lane1 // 32 == i, parts[i], o)
            of[8 * (GRP * b + g) : 8 * (GRP * b + g) + 8, :] = o
    tr = lax.broadcasted_iota(jnp.int32, (256, 256), 0) % TOK
    tc = lax.broadcasted_iota(jnp.int32, (256, 256), 1)
    tri = jnp.where((tc >= TOK) | (tr > tc), -1.0, 0.0).astype(bf16)

    R = 256

    def block(qt, b, qrow, carry, acc, diag):
        ks = b * 512
        if not isinstance(b, int):
            ks = pl.multiple_of(ks, 512)
        x = mm(qt, kk[pl.ds(ks, 512), :], 1, 1)
        e, a = [], []
        for g in range(GRP):
            ob = b * 32 + 8 * g
            if not isinstance(b, int):
                ob = pl.multiple_of(ob, 8)
            off = of[pl.ds(ob, 8), :][0:1, :]
            eg = jnp.exp2(jnp.minimum(x[:, 128 * g : 128 * g + 128] - off, score_cap))
            if diag:
                m = lax.broadcasted_iota(jnp.int32, (R, TOK), 1)
                t = lax.broadcasted_iota(jnp.int32, (R, TOK), 0)
                eg = jnp.where(GRP * m + g < t + qrow, eg, 0.0)
            e.append(eg)
            a.append(1.0 + eg)
        lg = jnp.log2((a[0] * a[1]) * (a[2] * a[3]))
        hi = lg.astype(bf16)
        lo = (lg - hi.astype(f32)).astype(bf16)
        cc = mm(jnp.concatenate([hi, lo], axis=1), tri)
        t = jnp.exp2((cc[:, 0:TOK] + carry) - lg)
        carry = carry + cc[:, TOK:]
        w0 = e[0] * t
        t = t * a[0]
        w1 = e[1] * t
        t = t * a[1]
        w2 = e[2] * t
        t = t * a[2]
        w3 = e[3] * t
        w = jnp.concatenate([u.astype(bf16) for u in (w0, w1, w2, w3)], axis=1)
        acc = acc + mm(w, vv[pl.ds(ks, 512), :])
        return carry, acc

    for j in range(2048 // R):
        qt = qq[R * j : R * j + R, :]
        carry = jnp.zeros((R, TOK), f32)
        acc = jnp.zeros((R, HD), f32)
        db = (R * j) // 512
        carry, acc = block(qt, db, R * j - 512 * db, carry, acc, True)
        for b in range(db - 1, -1, -1):
            carry, acc = block(qt, b, 0, carry, acc, False)
        n = acc * lax.rsqrt(jnp.mean(acc * acc, axis=1, keepdims=True) + eps_norm)
        n = n.astype(bf16)
        for d in range(R // TOK):
            lo_, hi_ = n[TOK * d : TOK * d + 64], n[TOK * d + 64 : TOK * d + TOK]
            out_ref[(R // TOK) * j + d] = jnp.concatenate([lo_, hi_], axis=1)


def attend(buf):
    return pl.pallas_call(
        attn_kernel,
        out_shape=jax.ShapeDtypeStruct((SRC, 64, TOK), bf16),
        scratch_shapes=[
            pltpu.VMEM((2048, 128), bf16),
            pltpu.VMEM((2048, 128), bf16),
            pltpu.VMEM((2048, HD), bf16),
            pltpu.VMEM((128, TOK), f32),
        ],
        compiler_params=pltpu.CompilerParams(vmem_limit_bytes=48 * 1024 * 1024),
    )(buf)


def gate_kernel(h_ref, w_ref, out_ref, o_ref):
    j = pl.program_id(0)
    first = jnp.concatenate([w_ref[i, :, 0:64] for i in range(4)], axis=1)
    o_ref[:, pl.ds(pl.multiple_of(256 * j, 256), 256)] = jnp.concatenate([w_ref[i, :, 64:128] for i in range(4)], axis=1)
    part = mm(h_ref[0], first, 1, 1)

    @pl.when(j == 0)
    def _():
        out_ref[...] = part

    @pl.when(j > 0)
    def _():
        out_ref[...] += part

    @pl.when(j == pl.num_programs(0) - 1)
    def _():
        v = out_ref[...]
        out_ref[...] = v / (1.0 + jnp.exp(-v))


def gate(hidden, w):
    return pl.pallas_call(
        gate_kernel,
        grid=(8,),
        in_specs=[
            pl.BlockSpec((1, TOK, 256), lambda j: (0, 0, j)),
            pl.BlockSpec((4, 1024, 128), lambda j: (j, 0, 0)),
        ],
        out_specs=[
            pl.BlockSpec((TOK, 1024), lambda j: (0, 0)),
            pl.BlockSpec((1024, 2048), lambda j: (0, 0)),
        ],
        out_shape=[jax.ShapeDtypeStruct((TOK, 1024), f32), jax.ShapeDtypeStruct((1024, 2048), bf16)],
        compiler_params=pltpu.CompilerParams(vmem_limit_bytes=32 * 1024 * 1024),
        cost_estimate=pl.CostEstimate(flops=2 * 128 * 1024 * 2048, bytes_accessed=12 << 20, transcendentals=1 << 17),
    )(hidden, w)


def mix_kernel(r_ref, g_ref, o_ref, out_ref, gd_ref):
    for h in range(0, SRC, 2):
        a, b = r_ref[h], r_ref[h + 1]
        top = jnp.concatenate([a[:, 0:HD], b[:, 0:HD]], axis=1)
        bot = jnp.concatenate([a[:, HD:], b[:, HD:]], axis=1)
        n = jnp.concatenate([top, bot], axis=0).astype(f32)
        s = slice(HD * h, HD * h + 2 * HD)
        gd_ref[:, s] = (n * g_ref[:, s]).astype(bf16)
    for j in range(4):
        s = slice(512 * j, 512 * j + 512)
        out_ref[0, :, s] = mm(gd_ref[...], o_ref[:, s]).astype(bf16)


def mix(ret, gact, o):
    return pl.pallas_call(
        mix_kernel,
        out_shape=jax.ShapeDtypeStruct((1, TOK, 2048), bf16),
        scratch_shapes=[pltpu.VMEM((TOK, 1024), bf16)],
        compiler_params=pltpu.CompilerParams(vmem_limit_bytes=32 * 1024 * 1024),
        cost_estimate=pl.CostEstimate(flops=2 * 128 * 1024 * 2048, bytes_accessed=6 << 20, transcendentals=0),
    )(ret, gact, o)


def shards(queries, key_rows, value_rows, break_offset, hidden_in, gate_weight, out_weight):
    joined = jnp.concatenate([gate_weight.T, out_weight], axis=1)
    joined = jnp.broadcast_to(joined[None], (SRC, 64, TOK))
    joined = lax.all_to_all(joined, "sp", split_axis=0, concat_axis=0, tiled=True)
    buf = pack(queries, key_rows, value_rows, break_offset)
    buf, joined = lax.optimization_barrier((buf, joined))
    w = lax.all_gather(joined.reshape(1, 1024, TOK), "dp", axis=0, tiled=True)
    buf = lax.all_to_all(buf, "sp", split_axis=0, concat_axis=0, tiled=True)
    heads = attend(buf)
    ret = lax.all_to_all(heads, "sp", split_axis=0, concat_axis=0, tiled=True)
    gact, o = gate(hidden_in, w)
    return mix(ret, gact, o)


def solution(mesh):
    tok = P("dp", "sp", None)
    return jax.shard_map(
        shards,
        mesh=mesh,
        in_specs=(tok, tok, tok, tok, tok, P("dp", "sp"), P("sp", "dp")),
        out_specs=tok,
        check_vma=False,
    )
```

```python
import math
import jax
import jax.numpy as jnp
from jax import lax
from jax.experimental import pallas as pl
from jax.experimental.pallas import tpu as pltpu
from jax.sharding import PartitionSpec as P


eps_norm = 1e-05
log2e = math.log2(math.e)
score_cap = 25.0
f32, bf16 = jnp.float32, jnp.bfloat16
SRC, TOK, HD, GRP = 16, 128, 64, 4
ROWS = TOK + TOK // 2 + 8


def mm(a, b, ca=1, cb=0):
    return lax.dot_general(a, b, (((ca,), (cb,)), ((), ())), preferred_element_type=f32)


def pack_kernel(q_ref, k_ref, v_ref, o_ref, gw_ref, ow_ref, out_ref, joined_ref):
    row = lax.broadcasted_iota(jnp.int32, (TOK, TOK), 0)
    col = lax.broadcasted_iota(jnp.int32, (TOK, TOK), 1)
    perm = jnp.where(col == GRP * (row % 32) + row // 32, 1.0, 0.0).astype(bf16)
    keys = mm(perm, k_ref[0]).astype(bf16)
    vals = mm(perm, v_ref[0]).astype(bf16)
    offs = mm(o_ref[0], perm, 1, 1).astype(bf16)
    eye = jnp.where(row[0:HD, 0:HD] == col[0:HD, 0:HD], 1.0, 0.0).astype(bf16)
    joined_ref[...] = jnp.concatenate([mm(gw_ref[...], eye, 0, 0).astype(bf16), ow_ref[...]], axis=1)
    for h in range(SRC):
        s = slice(HD * h, HD * h + HD)
        out_ref[h, 0:TOK, :] = jnp.concatenate([q_ref[0, :, s], keys[:, s]], axis=1)
        out_ref[h, TOK:192, :] = jnp.concatenate([vals[0:64, s], vals[64:128, s]], axis=1)
        out_ref[h, 192:200, :] = jnp.broadcast_to(offs[h : h + 1, :], (8, TOK))


def pack(q, k, v, o, gw, ow):
    return pl.pallas_call(
        pack_kernel,
        out_shape=[jax.ShapeDtypeStruct((SRC, ROWS, TOK), bf16), jax.ShapeDtypeStruct((HD, TOK), bf16)],
    )(q, k, v, o.transpose(0, 2, 1), gw, ow)


def attn_kernel(buf_ref, out_ref, qq, kk, vv, of):
    nblk = SRC // GRP
    for i in range(SRC):
        q = buf_ref[i, 0:TOK, 0:HD].astype(f32) * (log2e / 8.0)
        hi = q.astype(bf16)
        lo = (q - hi.astype(f32)).astype(bf16)
        qq[TOK * i : TOK * i + TOK, :] = jnp.concatenate([hi, lo], axis=1)
        for g in range(GRP):
            k = buf_ref[i, 32 * g : 32 * g + 32, HD : 2 * HD]
            r = 512 * (i // 4) + 128 * g + 32 * (i % 4)
            kk[r : r + 32, :] = jnp.concatenate([k, k], axis=1)
            vr = TOK + 32 * (g % 2)
            vv[r : r + 32, :] = buf_ref[i, vr : vr + 32, HD * (g // 2) : HD * (g // 2) + HD]
    lane1 = lax.broadcasted_iota(jnp.int32, (8, TOK), 1)
    for b in range(nblk):
        rows = [buf_ref[4 * b + i, 192:200, :].astype(f32) * log2e for i in range(4)]
        for g in range(GRP):
            parts = [r if (i == g) else pltpu.roll(r, (32 * (i - g)) % TOK, 1) for i, r in enumerate(rows)]
            o = parts[3]
            for i in range(3):
                o = jnp.where(lane1 // 32 == i, parts[i], o)
            of[8 * (GRP * b + g) : 8 * (GRP * b + g) + 8, :] = o
    tr = lax.broadcasted_iota(jnp.int32, (256, 256), 0) % TOK
    tc = lax.broadcasted_iota(jnp.int32, (256, 256), 1)
    tri = jnp.where((tc >= TOK) | (tr > tc), -1.0, 0.0).astype(bf16)

    R = 512

    def block(qt, b, qrow, carry, acc, diag):
        ks = b * 512
        if not isinstance(b, int):
            ks = pl.multiple_of(ks, 512)
        x = mm(qt, kk[pl.ds(ks, 512), :], 1, 1)
        e, a = [], []
        for g in range(GRP):
            ob = b * 32 + 8 * g
            if not isinstance(b, int):
                ob = pl.multiple_of(ob, 8)
            off = of[pl.ds(ob, 8), :][0:1, :]
            eg = jnp.exp2(jnp.minimum(x[:, 128 * g : 128 * g + 128] - off, score_cap))
            if diag:
                m = lax.broadcasted_iota(jnp.int32, (R, TOK), 1)
                t = lax.broadcasted_iota(jnp.int32, (R, TOK), 0)
                eg = jnp.where(GRP * m + g < t + qrow, eg, 0.0)
            e.append(eg)
            a.append(1.0 + eg)
        lg = jnp.log2((a[0] * a[1]) * (a[2] * a[3]))
        hi = lg.astype(bf16)
        lo = (lg - hi.astype(f32)).astype(bf16)
        cc = mm(jnp.concatenate([hi, lo], axis=1), tri)
        t = jnp.exp2((cc[:, 0:TOK] + carry) - lg)
        carry = carry + cc[:, TOK:]
        w0 = e[0] * t
        t = t * a[0]
        w1 = e[1] * t
        t = t * a[1]
        w2 = e[2] * t
        t = t * a[2]
        w3 = e[3] * t
        w = jnp.concatenate([u.astype(bf16) for u in (w0, w1, w2, w3)], axis=1)
        acc = acc + mm(w, vv[pl.ds(ks, 512), :])
        return carry, acc

    for j in range(2048 // R):
        qt = qq[R * j : R * j + R, :]
        carry = jnp.zeros((R, TOK), f32)
        acc = jnp.zeros((R, HD), f32)
        db = (R * j) // 512
        carry, acc = block(qt, db, R * j - 512 * db, carry, acc, True)
        for b in range(db - 1, -1, -1):
            carry, acc = block(qt, b, 0, carry, acc, False)
        n = acc * lax.rsqrt(jnp.mean(acc * acc, axis=1, keepdims=True) + eps_norm)
        n = n.astype(bf16)
        for d in range(R // TOK):
            lo_, hi_ = n[TOK * d : TOK * d + 64], n[TOK * d + 64 : TOK * d + TOK]
            out_ref[(R // TOK) * j + d] = jnp.concatenate([lo_, hi_], axis=1)


def attend(buf):
    return pl.pallas_call(
        attn_kernel,
        out_shape=jax.ShapeDtypeStruct((SRC, 64, TOK), bf16),
        scratch_shapes=[
            pltpu.VMEM((2048, 128), bf16),
            pltpu.VMEM((2048, 128), bf16),
            pltpu.VMEM((2048, HD), bf16),
            pltpu.VMEM((128, TOK), f32),
        ],
        compiler_params=pltpu.CompilerParams(vmem_limit_bytes=48 * 1024 * 1024),
    )(buf)


def gate_kernel(h_ref, w_ref, out_ref, o_ref):
    j = pl.program_id(0)
    first = jnp.concatenate([w_ref[i, :, 0:64] for i in range(4)], axis=1)
    o_ref[...] = jnp.concatenate([w_ref[i, :, 64:128] for i in range(4)], axis=1)
    part = mm(h_ref[0], first, 1, 1)

    @pl.when(j == 0)
    def _():
        out_ref[...] = part

    @pl.when(j > 0)
    def _():
        out_ref[...] += part

    @pl.when(j == pl.num_programs(0) - 1)
    def _():
        v = out_ref[...]
        out_ref[...] = v / (1.0 + jnp.exp(-v))


def gate(hidden, w):
    return pl.pallas_call(
        gate_kernel,
        grid=(8,),
        in_specs=[
            pl.BlockSpec((1, TOK, 256), lambda j: (0, 0, j)),
            pl.BlockSpec((4, 1024, 128), lambda j: (j, 0, 0)),
        ],
        out_specs=[
            pl.BlockSpec((TOK, 1024), lambda j: (0, 0)),
            pl.BlockSpec((1024, 256), lambda j: (0, j)),
        ],
        out_shape=[jax.ShapeDtypeStruct((TOK, 1024), f32), jax.ShapeDtypeStruct((1024, 2048), bf16)],
        compiler_params=pltpu.CompilerParams(vmem_limit_bytes=32 * 1024 * 1024),
        cost_estimate=pl.CostEstimate(flops=2 * 128 * 1024 * 2048, bytes_accessed=12 << 20, transcendentals=1 << 17),
    )(hidden, w)


def mix_kernel(r_ref, g_ref, o_ref, out_ref, gd_ref, ow_ref, sems):
    copies = [
        pltpu.make_async_copy(o_ref.at[:, 512 * j : 512 * j + 512], ow_ref.at[j], sems.at[j]) for j in range(4)
    ]
    for c in copies:
        c.start()
    for h in range(0, SRC, 2):
        a, b = r_ref[h], r_ref[h + 1]
        top = jnp.concatenate([a[:, 0:HD], b[:, 0:HD]], axis=1)
        bot = jnp.concatenate([a[:, HD:], b[:, HD:]], axis=1)
        n = jnp.concatenate([top, bot], axis=0).astype(f32)
        s = slice(HD * h, HD * h + 2 * HD)
        gd_ref[:, s] = (n * g_ref[:, s]).astype(bf16)
    for j in range(4):
        copies[j].wait()
        out_ref[0, :, 512 * j : 512 * j + 512] = mm(gd_ref[...], ow_ref[j]).astype(bf16)


def mix(ret, gact, o):
    return pl.pallas_call(
        mix_kernel,
        in_specs=[
            pl.BlockSpec(memory_space=pltpu.VMEM),
            pl.BlockSpec(memory_space=pltpu.VMEM),
            pl.BlockSpec(memory_space=pltpu.HBM),
        ],
        out_shape=jax.ShapeDtypeStruct((1, TOK, 2048), bf16),
        scratch_shapes=[
            pltpu.VMEM((TOK, 1024), bf16),
            pltpu.VMEM((4, 1024, 512), bf16),
            pltpu.SemaphoreType.DMA((4,)),
        ],
        compiler_params=pltpu.CompilerParams(vmem_limit_bytes=16 * 1024 * 1024),
        cost_estimate=pl.CostEstimate(flops=2 * 128 * 1024 * 2048, bytes_accessed=6 << 20, transcendentals=0),
    )(ret, gact, pltpu.with_memory_space_constraint(o, pltpu.HBM))


def shards(queries, key_rows, value_rows, break_offset, hidden_in, gate_weight, out_weight):
    buf, joined = pack(queries, key_rows, value_rows, break_offset, gate_weight, out_weight)
    joined = lax.all_gather(joined, "sp", axis=0, tiled=True)
    buf, joined = lax.optimization_barrier((buf, joined))
    w = lax.all_gather(joined.reshape(1, 1024, TOK), "dp", axis=0, tiled=True)
    buf = lax.all_to_all(buf, "sp", split_axis=0, concat_axis=0, tiled=True)
    heads = attend(buf)
    ret = lax.all_to_all(heads, "sp", split_axis=0, concat_axis=0, tiled=True)
    gact, o = gate(hidden_in, w)
    return mix(ret, gact, o)


def solution(mesh):
    tok = P("dp", "sp", None)
    return jax.shard_map(
        shards,
        mesh=mesh,
        in_specs=(tok, tok, tok, tok, tok, P("dp", "sp"), P("sp", "dp")),
        out_specs=tok,
        check_vma=False,
    )
```

```python
import math
import jax
import jax.numpy as jnp
from jax import lax
from jax.experimental import pallas as pl
from jax.experimental.pallas import tpu as pltpu
from jax.sharding import PartitionSpec as P


eps_norm = 1e-05
log2e = math.log2(math.e)
score_cap = 25.0
f32, bf16 = jnp.float32, jnp.bfloat16
SRC, TOK, HD, GRP = 16, 128, 64, 4
ROWS = TOK + TOK // 2 + 8


def mm(a, b, ca=1, cb=0):
    return lax.dot_general(a, b, (((ca,), (cb,)), ((), ())), preferred_element_type=f32)


def pack_kernel(q_ref, k_ref, v_ref, o_ref, gw_ref, ow_ref, out_ref, joined_ref):
    row = lax.broadcasted_iota(jnp.int32, (TOK, TOK), 0)
    col = lax.broadcasted_iota(jnp.int32, (TOK, TOK), 1)
    perm = jnp.where(col == GRP * (row % 32) + row // 32, 1.0, 0.0).astype(bf16)
    keys = mm(perm, k_ref[0]).astype(bf16)
    vals = mm(perm, v_ref[0]).astype(bf16)
    offs = mm(o_ref[0], perm, 1, 1).astype(bf16)
    eye = jnp.where(row[0:HD, 0:HD] == col[0:HD, 0:HD], 1.0, 0.0).astype(bf16)
    joined_ref[...] = jnp.concatenate([mm(gw_ref[...], eye, 0, 0).astype(bf16), ow_ref[...]], axis=1)
    for h in range(SRC):
        s = slice(HD * h, HD * h + HD)
        out_ref[h, 0:TOK, :] = jnp.concatenate([q_ref[0, :, s], keys[:, s]], axis=1)
        out_ref[h, TOK:192, :] = jnp.concatenate([vals[0:64, s], vals[64:128, s]], axis=1)
        out_ref[h, 192:200, :] = jnp.broadcast_to(offs[h : h + 1, :], (8, TOK))


def pack(q, k, v, o, gw, ow):
    return pl.pallas_call(
        pack_kernel,
        out_shape=[jax.ShapeDtypeStruct((SRC, ROWS, TOK), bf16), jax.ShapeDtypeStruct((HD, TOK), bf16)],
    )(q, k, v, o.transpose(0, 2, 1), gw, ow)


def attn_kernel(buf_ref, out_ref, qq, kk, vv, of):
    nblk = SRC // GRP
    for i in range(SRC):
        q = buf_ref[i, 0:TOK, 0:HD].astype(f32) * (log2e / 8.0)
        hi = q.astype(bf16)
        lo = (q - hi.astype(f32)).astype(bf16)
        qq[TOK * i : TOK * i + TOK, :] = jnp.concatenate([hi, lo], axis=1)
        for g in range(GRP):
            k = buf_ref[i, 32 * g : 32 * g + 32, HD : 2 * HD]
            r = 512 * (i // 4) + 128 * g + 32 * (i % 4)
            kk[r : r + 32, :] = jnp.concatenate([k, k], axis=1)
            vr = TOK + 32 * (g % 2)
            vv[r : r + 32, :] = buf_ref[i, vr : vr + 32, HD * (g // 2) : HD * (g // 2) + HD]
    lane1 = lax.broadcasted_iota(jnp.int32, (8, TOK), 1)
    for b in range(nblk):
        rows = [buf_ref[4 * b + i, 192:200, :].astype(f32) * log2e for i in range(4)]
        for g in range(GRP):
            parts = [r if (i == g) else pltpu.roll(r, (32 * (i - g)) % TOK, 1) for i, r in enumerate(rows)]
            o = parts[3]
            for i in range(3):
                o = jnp.where(lane1 // 32 == i, parts[i], o)
            of[8 * (GRP * b + g) : 8 * (GRP * b + g) + 8, :] = o
    tr = lax.broadcasted_iota(jnp.int32, (256, 256), 0) % TOK
    tc = lax.broadcasted_iota(jnp.int32, (256, 256), 1)
    tri = jnp.where((tc >= TOK) | (tr > tc), -1.0, 0.0).astype(bf16)

    R = 512

    def block(qt, b, qrow, carry, acc, diag):
        ks = b * 512
        if not isinstance(b, int):
            ks = pl.multiple_of(ks, 512)
        x = mm(qt, kk[pl.ds(ks, 512), :], 1, 1)
        e, a = [], []
        for g in range(GRP):
            ob = b * 32 + 8 * g
            if not isinstance(b, int):
                ob = pl.multiple_of(ob, 8)
            off = of[pl.ds(ob, 8), :][0:1, :]
            eg = jnp.exp2(jnp.minimum(x[:, 128 * g : 128 * g + 128] - off, score_cap))
            if diag:
                m = lax.broadcasted_iota(jnp.int32, (R, TOK), 1)
                t = lax.broadcasted_iota(jnp.int32, (R, TOK), 0)
                eg = jnp.where(GRP * m + g < t + qrow, eg, 0.0)
            e.append(eg)
            a.append(1.0 + eg)
        lg = jnp.log2((a[0] * a[1]) * (a[2] * a[3]))
        hi = lg.astype(bf16)
        lo = (lg - hi.astype(f32)).astype(bf16)
        cc = mm(jnp.concatenate([hi, lo], axis=1), tri)
        t = jnp.exp2((cc[:, 0:TOK] + carry) - lg)
        carry = carry + cc[:, TOK:]
        w0 = e[0] * t
        t = t * a[0]
        w1 = e[1] * t
        t = t * a[1]
        w2 = e[2] * t
        t = t * a[2]
        w3 = e[3] * t
        w = jnp.concatenate([u.astype(bf16) for u in (w0, w1, w2, w3)], axis=1)
        acc = acc + mm(w, vv[pl.ds(ks, 512), :])
        return carry, acc

    for j in range(2048 // R):
        qt = qq[R * j : R * j + R, :]
        carry = jnp.zeros((R, TOK), f32)
        acc = jnp.zeros((R, HD), f32)
        db = (R * j) // 512
        carry, acc = block(qt, db, R * j - 512 * db, carry, acc, True)
        for b in range(db - 1, -1, -1):
            carry, acc = block(qt, b, 0, carry, acc, False)
        n = acc * lax.rsqrt(jnp.mean(acc * acc, axis=1, keepdims=True) + eps_norm)
        n = n.astype(bf16)
        for d in range(R // TOK):
            lo_, hi_ = n[TOK * d : TOK * d + 64], n[TOK * d + 64 : TOK * d + TOK]
            out_ref[(R // TOK) * j + d] = jnp.concatenate([lo_, hi_], axis=1)


def attend(buf):
    return pl.pallas_call(
        attn_kernel,
        out_shape=jax.ShapeDtypeStruct((SRC, 64, TOK), bf16),
        scratch_shapes=[
            pltpu.VMEM((2048, 128), bf16),
            pltpu.VMEM((2048, 128), bf16),
            pltpu.VMEM((2048, HD), bf16),
            pltpu.VMEM((128, TOK), f32),
        ],
        compiler_params=pltpu.CompilerParams(vmem_limit_bytes=48 * 1024 * 1024),
    )(buf)


def gate_kernel(h_ref, w_ref, out_ref, o_ref):
    j = pl.program_id(0)
    first = jnp.concatenate([w_ref[i, :, 0:64] for i in range(4)], axis=1)
    o_ref[0] = jnp.concatenate([w_ref[i, :, 64:128] for i in range(4)], axis=1)
    part = mm(h_ref[0], first, 1, 1)

    @pl.when(j == 0)
    def _():
        out_ref[...] = part

    @pl.when(j > 0)
    def _():
        out_ref[...] += part

    @pl.when(j == pl.num_programs(0) - 1)
    def _():
        v = out_ref[...]
        out_ref[...] = v / (1.0 + jnp.exp(-v))


def gate(hidden, w):
    return pl.pallas_call(
        gate_kernel,
        grid=(8,),
        in_specs=[
            pl.BlockSpec((1, TOK, 256), lambda j: (0, 0, j)),
            pl.BlockSpec((4, 1024, 128), lambda j: (j, 0, 0)),
        ],
        out_specs=[
            pl.BlockSpec((TOK, 1024), lambda j: (0, 0)),
            pl.BlockSpec((1, 1024, 256), lambda j: (j, 0, 0)),
        ],
        out_shape=[jax.ShapeDtypeStruct((TOK, 1024), f32), pltpu.HBM((8, 1024, 256), bf16)],
        compiler_params=pltpu.CompilerParams(vmem_limit_bytes=32 * 1024 * 1024),
        cost_estimate=pl.CostEstimate(flops=2 * 128 * 1024 * 2048, bytes_accessed=12 << 20, transcendentals=1 << 17),
    )(pltpu.with_memory_space_constraint(hidden, pltpu.HBM), pltpu.with_memory_space_constraint(w, pltpu.HBM))


def mix_kernel(r_ref, g_ref, o_ref, out_ref, gd_ref, ow_ref, sems):
    copies = [pltpu.make_async_copy(o_ref.at[j], ow_ref.at[j], sems.at[j]) for j in range(8)]
    for c in copies:
        c.start()
    for h in range(0, SRC, 2):
        a, b = r_ref[h], r_ref[h + 1]
        top = jnp.concatenate([a[:, 0:HD], b[:, 0:HD]], axis=1)
        bot = jnp.concatenate([a[:, HD:], b[:, HD:]], axis=1)
        n = jnp.concatenate([top, bot], axis=0).astype(f32)
        s = slice(HD * h, HD * h + 2 * HD)
        gd_ref[:, s] = (n * g_ref[:, s]).astype(bf16)
    for j in range(8):
        copies[j].wait()
        out_ref[0, :, 256 * j : 256 * j + 256] = mm(gd_ref[...], ow_ref[j]).astype(bf16)


def mix(ret, gact, o):
    return pl.pallas_call(
        mix_kernel,
        in_specs=[
            pl.BlockSpec(memory_space=pltpu.VMEM),
            pl.BlockSpec(memory_space=pltpu.VMEM),
            pl.BlockSpec(memory_space=pltpu.HBM),
        ],
        out_shape=jax.ShapeDtypeStruct((1, TOK, 2048), bf16),
        scratch_shapes=[
            pltpu.VMEM((TOK, 1024), bf16),
            pltpu.VMEM((8, 1024, 256), bf16),
            pltpu.SemaphoreType.DMA((8,)),
        ],
        compiler_params=pltpu.CompilerParams(vmem_limit_bytes=16 * 1024 * 1024),
        cost_estimate=pl.CostEstimate(flops=2 * 128 * 1024 * 2048, bytes_accessed=6 << 20, transcendentals=0),
    )(ret, gact, pltpu.with_memory_space_constraint(o, pltpu.HBM))


def shards(queries, key_rows, value_rows, break_offset, hidden_in, gate_weight, out_weight):
    buf, joined = pack(queries, key_rows, value_rows, break_offset, gate_weight, out_weight)
    joined = lax.all_gather(joined, "sp", axis=0, tiled=True)
    buf, joined = lax.optimization_barrier((buf, joined))
    w = lax.all_gather(joined.reshape(1, 1024, TOK), "dp", axis=0, tiled=True)
    buf = lax.all_to_all(buf, "sp", split_axis=0, concat_axis=0, tiled=True)
    heads = attend(buf)
    ret = lax.all_to_all(heads, "sp", split_axis=0, concat_axis=0, tiled=True)
    gact, o = gate(hidden_in, w)
    return mix(ret, gact, o)


def solution(mesh):
    tok = P("dp", "sp", None)
    return jax.shard_map(
        shards,
        mesh=mesh,
        in_specs=(tok, tok, tok, tok, tok, P("dp", "sp"), P("sp", "dp")),
        out_specs=tok,
        check_vma=False,
    )
```

```python
import math
import jax
import jax.numpy as jnp
from jax import lax
from jax.experimental import pallas as pl
from jax.experimental.pallas import tpu as pltpu
from jax.sharding import PartitionSpec as P


eps_norm = 1e-05
log2e = math.log2(math.e)
score_cap = 25.0
f32, bf16 = jnp.float32, jnp.bfloat16
SRC, TOK, HD, GRP = 16, 128, 64, 4
ROWS = TOK + TOK // 2 + 8


def mm(a, b, ca=1, cb=0):
    return lax.dot_general(a, b, (((ca,), (cb,)), ((), ())), preferred_element_type=f32)


def pack_kernel(q_ref, k_ref, v_ref, o_ref, gw_ref, ow_ref, out_ref, joined_ref):
    row = lax.broadcasted_iota(jnp.int32, (TOK, TOK), 0)
    col = lax.broadcasted_iota(jnp.int32, (TOK, TOK), 1)
    perm = jnp.where(col == GRP * (row % 32) + row // 32, 1.0, 0.0).astype(bf16)
    keys = mm(perm, k_ref[0]).astype(bf16)
    vals = mm(perm, v_ref[0]).astype(bf16)
    offs = mm(o_ref[0], perm, 1, 1).astype(bf16)
    eye = jnp.where(row[0:HD, 0:HD] == col[0:HD, 0:HD], 1.0, 0.0).astype(bf16)
    joined_ref[...] = jnp.concatenate([mm(gw_ref[...], eye, 0, 0).astype(bf16), ow_ref[...]], axis=1)
    for h in range(SRC):
        s = slice(HD * h, HD * h + HD)
        out_ref[h, 0:TOK, :] = jnp.concatenate([q_ref[0, :, s], keys[:, s]], axis=1)
        out_ref[h, TOK:192, :] = jnp.concatenate([vals[0:64, s], vals[64:128, s]], axis=1)
        out_ref[h, 192:200, :] = jnp.broadcast_to(offs[h : h + 1, :], (8, TOK))


def pack(q, k, v, o, gw, ow):
    return pl.pallas_call(
        pack_kernel,
        out_shape=[jax.ShapeDtypeStruct((SRC, ROWS, TOK), bf16), jax.ShapeDtypeStruct((HD, TOK), bf16)],
    )(q, k, v, o.transpose(0, 2, 1), gw, ow)


def attn_kernel(buf_ref, out_ref, qq, kk, vv, of):
    nblk = SRC // GRP
    for i in range(SRC):
        q = buf_ref[i, 0:TOK, 0:HD].astype(f32) * (log2e / 8.0)
        hi = q.astype(bf16)
        lo = (q - hi.astype(f32)).astype(bf16)
        qq[TOK * i : TOK * i + TOK, :] = jnp.concatenate([hi, lo], axis=1)
        for g in range(GRP):
            k = buf_ref[i, 32 * g : 32 * g + 32, HD : 2 * HD]
            r = 512 * (i // 4) + 128 * g + 32 * (i % 4)
            kk[r : r + 32, :] = jnp.concatenate([k, k], axis=1)
            vr = TOK + 32 * (g % 2)
            vv[r : r + 32, :] = buf_ref[i, vr : vr + 32, HD * (g // 2) : HD * (g // 2) + HD]
    lane1 = lax.broadcasted_iota(jnp.int32, (8, TOK), 1)
    for b in range(nblk):
        rows = [buf_ref[4 * b + i, 192:200, :].astype(f32) * log2e for i in range(4)]
        for g in range(GRP):
            parts = [r if (i == g) else pltpu.roll(r, (32 * (i - g)) % TOK, 1) for i, r in enumerate(rows)]
            o = parts[3]
            for i in range(3):
                o = jnp.where(lane1 // 32 == i, parts[i], o)
            of[8 * (GRP * b + g) : 8 * (GRP * b + g) + 8, :] = o
    tr = lax.broadcasted_iota(jnp.int32, (256, 256), 0) % TOK
    tc = lax.broadcasted_iota(jnp.int32, (256, 256), 1)
    tri = jnp.where((tc >= TOK) | (tr > tc), -1.0, 0.0).astype(bf16)

    R = 512

    def block(qt, b, qrow, carry, acc, diag):
        ks = b * 512
        if not isinstance(b, int):
            ks = pl.multiple_of(ks, 512)
        x = mm(qt, kk[pl.ds(ks, 512), :], 1, 1)
        e, a = [], []
        for g in range(GRP):
            ob = b * 32 + 8 * g
            if not isinstance(b, int):
                ob = pl.multiple_of(ob, 8)
            off = of[pl.ds(ob, 8), :][0:1, :]
            eg = jnp.exp2(jnp.minimum(x[:, 128 * g : 128 * g + 128] - off, score_cap))
            if diag:
                m = lax.broadcasted_iota(jnp.int32, (R, TOK), 1)
                t = lax.broadcasted_iota(jnp.int32, (R, TOK), 0)
                eg = jnp.where(GRP * m + g < t + qrow, eg, 0.0)
            e.append(eg)
            a.append(1.0 + eg)
        lg = jnp.log2((a[0] * a[1]) * (a[2] * a[3]))
        hi = lg.astype(bf16)
        lo = (lg - hi.astype(f32)).astype(bf16)
        cc = mm(jnp.concatenate([hi, lo], axis=1), tri)
        t = jnp.exp2((cc[:, 0:TOK] + carry) - lg)
        carry = carry + cc[:, TOK:]
        w0 = e[0] * t
        t = t * a[0]
        w1 = e[1] * t
        t = t * a[1]
        w2 = e[2] * t
        t = t * a[2]
        w3 = e[3] * t
        w = jnp.concatenate([u.astype(bf16) for u in (w0, w1, w2, w3)], axis=1)
        acc = acc + mm(w, vv[pl.ds(ks, 512), :])
        return carry, acc

    for j in range(2048 // R):
        qt = qq[R * j : R * j + R, :]
        carry = jnp.zeros((R, TOK), f32)
        acc = jnp.zeros((R, HD), f32)
        db = (R * j) // 512
        carry, acc = block(qt, db, R * j - 512 * db, carry, acc, True)
        for b in range(db - 1, -1, -1):
            carry, acc = block(qt, b, 0, carry, acc, False)
        n = acc * lax.rsqrt(jnp.mean(acc * acc, axis=1, keepdims=True) + eps_norm)
        n = n.astype(bf16)
        for d in range(R // TOK):
            lo_, hi_ = n[TOK * d : TOK * d + 64], n[TOK * d + 64 : TOK * d + TOK]
            out_ref[(R // TOK) * j + d] = jnp.concatenate([lo_, hi_], axis=1)


def attend(buf):
    return pl.pallas_call(
        attn_kernel,
        out_shape=jax.ShapeDtypeStruct((SRC, 64, TOK), bf16),
        scratch_shapes=[
            pltpu.VMEM((2048, 128), bf16),
            pltpu.VMEM((2048, 128), bf16),
            pltpu.VMEM((2048, HD), bf16),
            pltpu.VMEM((128, TOK), f32),
        ],
        compiler_params=pltpu.CompilerParams(vmem_limit_bytes=48 * 1024 * 1024),
    )(buf)


def turn_kernel(x_ref, out_ref):
    out_ref[...] = x_ref[...].T


def turn(x):
    return pl.pallas_call(turn_kernel, out_shape=jax.ShapeDtypeStruct((128, 1024), bf16))(x)


def two_chips(pos_ref, own_ref, sib_ref, j):
    p = pos_ref[0]
    south, x, y = (p & 1) == 0, (p >> 1) & 3, p >> 3
    rows = []
    for chip in (2 * j, 2 * j + 1):
        dy, dx = (y - chip // 4) & 3, (x - chip % 4) & 3
        first, second = 4 * dy + dx, 4 * dx + dy
        a = own_ref[jnp.where(south, first, second)]
        b = sib_ref[jnp.where(south, second, first)]
        rows += [jnp.where(south, a, b), jnp.where(south, b, a)]
    return jnp.concatenate(rows, axis=0)


def gate_kernel(pos_ref, h_ref, own_ref, sib_ref, out_ref):
    acc = jnp.zeros((TOK, 1024), f32)
    for j in range(8):
        acc = acc + mm(h_ref[0, :, 256 * j : 256 * j + 256], two_chips(pos_ref, own_ref, sib_ref, j))
    out_ref[...] = acc / (1.0 + jnp.exp(-acc))


def mix_kernel(pos_ref, r_ref, g_ref, own_ref, sib_ref, out_ref, gd_ref):
    for h in range(0, SRC, 2):
        a, b = r_ref[h], r_ref[h + 1]
        top = jnp.concatenate([a[:, 0:HD], b[:, 0:HD]], axis=1)
        bot = jnp.concatenate([a[:, HD:], b[:, HD:]], axis=1)
        n = jnp.concatenate([top, bot], axis=0).astype(f32)
        s = slice(HD * h, HD * h + 2 * HD)
        gd_ref[:, s] = (n * g_ref[:, s]).astype(bf16)
    for j in range(8):
        w = two_chips(pos_ref, own_ref, sib_ref, j)
        out_ref[0, :, 256 * j : 256 * j + 256] = mm(gd_ref[...], w, 1, 1).astype(bf16)


def whole(n, smem=1):
    spec = [pl.BlockSpec(memory_space=pltpu.SMEM)] * smem
    return spec + [pl.BlockSpec(memory_space=pltpu.VMEM)] * n


def gate(tab, hidden, own, sib):
    return pl.pallas_call(
        gate_kernel,
        in_specs=whole(3),
        out_shape=jax.ShapeDtypeStruct((TOK, 1024), f32),
        compiler_params=pltpu.CompilerParams(vmem_limit_bytes=40 * 1024 * 1024),
        cost_estimate=pl.CostEstimate(flops=2 * 128 * 1024 * 2048, bytes_accessed=5 << 20, transcendentals=1 << 17),
    )(tab, hidden, own, sib)


def mix(tab, ret, gact, own, sib):
    return pl.pallas_call(
        mix_kernel,
        in_specs=whole(4),
        out_shape=jax.ShapeDtypeStruct((1, TOK, 2048), bf16),
        scratch_shapes=[pltpu.VMEM((TOK, 1024), bf16)],
        compiler_params=pltpu.CompilerParams(vmem_limit_bytes=40 * 1024 * 1024),
        cost_estimate=pl.CostEstimate(flops=2 * 128 * 1024 * 2048, bytes_accessed=6 << 20, transcendentals=0),
    )(tab, ret, gact, own, sib)


def moves(phase, step):
    out = []
    for y in range(4):
        for x in range(4):
            for c in range(2):
                along_x = (c == 0) == (phase == 1)
                ty, tx = (y, (x + step) % 4) if along_x else ((y + step) % 4, x)
                out.append(((y * 4 + x) * 2 + c, (ty * 4 + tx) * 2 + c))
    return out


def ring(b, phase):
    back1 = lax.ppermute(b, "dp", moves(phase, 1))
    back3 = lax.ppermute(b, "dp", moves(phase, -1))
    top = lax.ppermute(b[..., :64, :], "dp", moves(phase, 2))
    bot = lax.ppermute(b[..., 64:, :], "dp", moves(phase, -2))
    return back1, back3, top, bot


def shards(queries, key_rows, value_rows, break_offset, hidden_in, gate_weight, out_weight):
    buf, joined = pack(queries, key_rows, value_rows, break_offset, gate_weight, out_weight)
    joined = lax.all_gather(joined, "sp", axis=0, tiled=True)
    buf, joined = lax.optimization_barrier((buf, joined))
    buf = lax.all_to_all(buf, "sp", split_axis=0, concat_axis=0, tiled=True)
    b = turn(joined)
    back1, back3, top, bot = ring(b, 1)
    b = jnp.stack([b, back1, jnp.concatenate([top, bot], axis=0), back3])
    back1, back3, top, bot = ring(b, 2)
    own_g = jnp.concatenate([b[:, :64], back1[:, :64], top, back3[:, :64]], axis=0)
    own_o = jnp.concatenate([b[:, 64:], back1[:, 64:], bot, back3[:, 64:]], axis=0)
    swap = [(p, p ^ 1) for p in range(32)]
    sib_g = lax.ppermute(own_g, "dp", swap)
    sib_o = lax.ppermute(own_o, "dp", swap)
    pos = lax.axis_index("dp").astype(jnp.int32).reshape(1)
    heads = attend(buf)
    ret = lax.all_to_all(heads, "sp", split_axis=0, concat_axis=0, tiled=True)
    gact = gate(pos, hidden_in, own_g, sib_g)
    return mix(pos, ret, gact, own_o, sib_o)


def solution(mesh):
    tok = P("dp", "sp", None)
    return jax.shard_map(
        shards,
        mesh=mesh,
        in_specs=(tok, tok, tok, tok, tok, P("dp", "sp"), P("sp", "dp")),
        out_specs=tok,
        check_vma=False,
    )
```

```python
import math
import jax
import jax.numpy as jnp
from jax import lax
from jax.experimental import pallas as pl
from jax.experimental.pallas import tpu as pltpu
from jax.sharding import PartitionSpec as P


eps_norm = 1e-05
log2e = math.log2(math.e)
score_cap = 25.0
f32, bf16 = jnp.float32, jnp.bfloat16
SRC, TOK, HD, GRP = 16, 128, 64, 4
ROWS = TOK + TOK // 2 + 8


def mm(a, b, ca=1, cb=0):
    return lax.dot_general(a, b, (((ca,), (cb,)), ((), ())), preferred_element_type=f32)


def pack_kernel(q_ref, k_ref, v_ref, o_ref, gw_ref, ow_ref, out_ref, joined_ref):
    row = lax.broadcasted_iota(jnp.int32, (TOK, TOK), 0)
    col = lax.broadcasted_iota(jnp.int32, (TOK, TOK), 1)
    perm = jnp.where(col == GRP * (row % 32) + row // 32, 1.0, 0.0).astype(bf16)
    keys = mm(perm, k_ref[0]).astype(bf16)
    vals = mm(perm, v_ref[0]).astype(bf16)
    offs = mm(o_ref[0], perm, 1, 1).astype(bf16)
    eye = jnp.where(row[0:HD, 0:HD] == col[0:HD, 0:HD], 1.0, 0.0).astype(bf16)
    joined_ref[...] = jnp.concatenate([mm(gw_ref[...], eye, 0, 0).astype(bf16), ow_ref[...]], axis=1)
    for h in range(SRC):
        s = slice(HD * h, HD * h + HD)
        out_ref[h, 0:TOK, :] = jnp.concatenate([q_ref[0, :, s], keys[:, s]], axis=1)
        out_ref[h, TOK:192, :] = jnp.concatenate([vals[0:64, s], vals[64:128, s]], axis=1)
        out_ref[h, 192:200, :] = jnp.broadcast_to(offs[h : h + 1, :], (8, TOK))


def pack(q, k, v, o, gw, ow):
    return pl.pallas_call(
        pack_kernel,
        out_shape=[jax.ShapeDtypeStruct((SRC, ROWS, TOK), bf16), jax.ShapeDtypeStruct((HD, TOK), bf16)],
    )(q, k, v, o.transpose(0, 2, 1), gw, ow)


def attn_kernel(buf_ref, out_ref, qq, kk, vv, of):
    nblk = SRC // GRP
    for i in range(SRC):
        q = buf_ref[i, 0:TOK, 0:HD].astype(f32) * (log2e / 8.0)
        hi = q.astype(bf16)
        lo = (q - hi.astype(f32)).astype(bf16)
        qq[TOK * i : TOK * i + TOK, :] = jnp.concatenate([hi, lo], axis=1)
        for g in range(GRP):
            k = buf_ref[i, 32 * g : 32 * g + 32, HD : 2 * HD]
            r = 512 * (i // 4) + 128 * g + 32 * (i % 4)
            kk[r : r + 32, :] = jnp.concatenate([k, k], axis=1)
            vr = TOK + 32 * (g % 2)
            vv[r : r + 32, :] = buf_ref[i, vr : vr + 32, HD * (g // 2) : HD * (g // 2) + HD]
    lane1 = lax.broadcasted_iota(jnp.int32, (8, TOK), 1)
    for b in range(nblk):
        rows = [buf_ref[4 * b + i, 192:200, :].astype(f32) * log2e for i in range(4)]
        for g in range(GRP):
            parts = [r if (i == g) else pltpu.roll(r, (32 * (i - g)) % TOK, 1) for i, r in enumerate(rows)]
            o = parts[3]
            for i in range(3):
                o = jnp.where(lane1 // 32 == i, parts[i], o)
            of[8 * (GRP * b + g) : 8 * (GRP * b + g) + 8, :] = o
    tr = lax.broadcasted_iota(jnp.int32, (256, 256), 0) % TOK
    tc = lax.broadcasted_iota(jnp.int32, (256, 256), 1)
    tri = jnp.where((tc >= TOK) | (tr > tc), -1.0, 0.0).astype(bf16)

    R = 512

    def block(qt, b, qrow, carry, acc, diag):
        ks = b * 512
        if not isinstance(b, int):
            ks = pl.multiple_of(ks, 512)
        x = mm(qt, kk[pl.ds(ks, 512), :], 1, 1)
        e, a = [], []
        for g in range(GRP):
            ob = b * 32 + 8 * g
            if not isinstance(b, int):
                ob = pl.multiple_of(ob, 8)
            off = of[pl.ds(ob, 8), :][0:1, :]
            eg = jnp.exp2(jnp.minimum(x[:, 128 * g : 128 * g + 128] - off, score_cap))
            if diag:
                m = lax.broadcasted_iota(jnp.int32, (R, TOK), 1)
                t = lax.broadcasted_iota(jnp.int32, (R, TOK), 0)
                eg = jnp.where(GRP * m + g < t + qrow, eg, 0.0)
            e.append(eg)
            a.append(1.0 + eg)
        lg = jnp.log2((a[0] * a[1]) * (a[2] * a[3]))
        hi = lg.astype(bf16)
        lo = (lg - hi.astype(f32)).astype(bf16)
        cc = mm(jnp.concatenate([hi, lo], axis=1), tri)
        t = jnp.exp2((cc[:, 0:TOK] + carry) - lg)
        carry = carry + cc[:, TOK:]
        w0 = e[0] * t
        t = t * a[0]
        w1 = e[1] * t
        t = t * a[1]
        w2 = e[2] * t
        t = t * a[2]
        w3 = e[3] * t
        w = jnp.concatenate([u.astype(bf16) for u in (w0, w1, w2, w3)], axis=1)
        acc = acc + mm(w, vv[pl.ds(ks, 512), :])
        return carry, acc

    for j in range(2048 // R):
        qt = qq[R * j : R * j + R, :]
        carry = jnp.zeros((R, TOK), f32)
        acc = jnp.zeros((R, HD), f32)
        db = (R * j) // 512
        carry, acc = block(qt, db, R * j - 512 * db, carry, acc, True)
        for b in range(db - 1, -1, -1):
            carry, acc = block(qt, b, 0, carry, acc, False)
        n = acc * lax.rsqrt(jnp.mean(acc * acc, axis=1, keepdims=True) + eps_norm)
        n = n.astype(bf16)
        for d in range(R // TOK):
            lo_, hi_ = n[TOK * d : TOK * d + 64], n[TOK * d + 64 : TOK * d + TOK]
            out_ref[(R // TOK) * j + d] = jnp.concatenate([lo_, hi_], axis=1)


def attend(buf):
    return pl.pallas_call(
        attn_kernel,
        out_shape=jax.ShapeDtypeStruct((SRC, 64, TOK), bf16),
        scratch_shapes=[
            pltpu.VMEM((2048, 128), bf16),
            pltpu.VMEM((2048, 128), bf16),
            pltpu.VMEM((2048, HD), bf16),
            pltpu.VMEM((128, TOK), f32),
        ],
        compiler_params=pltpu.CompilerParams(vmem_limit_bytes=48 * 1024 * 1024),
    )(buf)


def turn_kernel(x_ref, out_ref):
    out_ref[...] = x_ref[...].T


def turn(x):
    return pl.pallas_call(turn_kernel, out_shape=jax.ShapeDtypeStruct((128, 1024), bf16))(x)


def fetch(pos_ref, own_ref, sib_ref, w_ref, sems, half):
    p = pos_ref[0]
    core, x, y = p & 1, (p >> 1) & 3, p >> 3
    copies = []
    for chip in range(16):
        dy, dx = (y - chip // 4) & 3, (x - chip % 4) & 3
        first, second = 4 * dy + dx, 4 * dx + dy
        mine = first + core * (second - first)
        other = second + core * (first - second)
        for k, (ref, slot, c) in enumerate(((own_ref, mine, core), (sib_ref, other, 1 - core))):
            dst = w_ref.at[chip, c]
            copies.append(pltpu.make_async_copy(ref.at[slot, half], dst, sems.at[2 * chip + k]))
    for c in copies:
        c.start()
    return copies


def gate_kernel(pos_ref, h_ref, own_ref, sib_ref, out_ref, w_ref, sems):
    copies = fetch(pos_ref, own_ref, sib_ref, w_ref, sems, 0)
    acc = jnp.zeros((TOK, 1024), f32)
    for j in range(8):
        for c in copies[4 * j : 4 * j + 4]:
            c.wait()
        acc = acc + mm(h_ref[0, :, 256 * j : 256 * j + 256], w_ref[2 * j : 2 * j + 2].reshape(256, 1024))
    out_ref[...] = acc / (1.0 + jnp.exp(-acc))


def mix_kernel(pos_ref, r_ref, g_ref, own_ref, sib_ref, out_ref, gd_ref, w_ref, sems):
    copies = fetch(pos_ref, own_ref, sib_ref, w_ref, sems, 1)
    for h in range(0, SRC, 2):
        a, b = r_ref[h], r_ref[h + 1]
        top = jnp.concatenate([a[:, 0:HD], b[:, 0:HD]], axis=1)
        bot = jnp.concatenate([a[:, HD:], b[:, HD:]], axis=1)
        n = jnp.concatenate([top, bot], axis=0).astype(f32)
        s = slice(HD * h, HD * h + 2 * HD)
        gd_ref[:, s] = (n * g_ref[:, s]).astype(bf16)
    for j in range(8):
        for c in copies[4 * j : 4 * j + 4]:
            c.wait()
        w = w_ref[2 * j : 2 * j + 2].reshape(256, 1024)
        out_ref[0, :, 256 * j : 256 * j + 256] = mm(gd_ref[...], w, 1, 1).astype(bf16)


def specs(n):
    vmem = [pl.BlockSpec(memory_space=pltpu.VMEM)] * n
    return [pl.BlockSpec(memory_space=pltpu.SMEM)] + vmem + [pl.BlockSpec(memory_space=pltpu.HBM)] * 2


def gate(pos, hidden, own, sib):
    return pl.pallas_call(
        gate_kernel,
        in_specs=specs(1),
        out_shape=jax.ShapeDtypeStruct((TOK, 1024), f32),
        scratch_shapes=[pltpu.VMEM((16, 2, 64, 1024), bf16), pltpu.SemaphoreType.DMA((32,))],
        compiler_params=pltpu.CompilerParams(vmem_limit_bytes=24 * 1024 * 1024),
        cost_estimate=pl.CostEstimate(flops=2 * 128 * 1024 * 2048, bytes_accessed=5 << 20, transcendentals=1 << 17),
    )(pos, hidden, own, sib)


def mix(pos, ret, gact, own, sib):
    return pl.pallas_call(
        mix_kernel,
        in_specs=specs(2),
        out_shape=jax.ShapeDtypeStruct((1, TOK, 2048), bf16),
        scratch_shapes=[
            pltpu.VMEM((TOK, 1024), bf16),
            pltpu.VMEM((16, 2, 64, 1024), bf16),
            pltpu.SemaphoreType.DMA((32,)),
        ],
        compiler_params=pltpu.CompilerParams(vmem_limit_bytes=24 * 1024 * 1024),
        cost_estimate=pl.CostEstimate(flops=2 * 128 * 1024 * 2048, bytes_accessed=6 << 20, transcendentals=0),
    )(pos, ret, gact, own, sib)


def moves(phase, step):
    out = []
    for y in range(4):
        for x in range(4):
            for c in range(2):
                along_x = (c == 0) == (phase == 1)
                ty, tx = (y, (x + step) % 4) if along_x else ((y + step) % 4, x)
                out.append(((y * 4 + x) * 2 + c, (ty * 4 + tx) * 2 + c))
    return out


def ring(b, phase):
    back1 = lax.ppermute(b, "dp", moves(phase, 1))
    back3 = lax.ppermute(b, "dp", moves(phase, -1))
    top = lax.ppermute(b[..., :64, :], "dp", moves(phase, 2))
    bot = lax.ppermute(b[..., 64:, :], "dp", moves(phase, -2))
    return back1, back3, top, bot


def shards(queries, key_rows, value_rows, break_offset, hidden_in, gate_weight, out_weight):
    buf, joined = pack(queries, key_rows, value_rows, break_offset, gate_weight, out_weight)
    joined = lax.all_gather(joined, "sp", axis=0, tiled=True)
    buf, joined = lax.optimization_barrier((buf, joined))
    buf = lax.all_to_all(buf, "sp", split_axis=0, concat_axis=0, tiled=True)
    b = turn(joined)
    back1, back3, top, bot = ring(b, 1)
    b = jnp.stack([b, back1, jnp.concatenate([top, bot], axis=0), back3])
    back1, back3, top, bot = ring(b, 2)
    own = jnp.stack([b, back1, jnp.concatenate([top, bot], axis=1), back3])
    sib = lax.ppermute(own, "dp", [(p, p ^ 1) for p in range(32)])
    own, sib = (
        pltpu.with_memory_space_constraint(w.reshape(16, 2, 64, 1024), pltpu.HBM) for w in (own, sib)
    )
    pos = lax.axis_index("dp").astype(jnp.int32).reshape(1)
    heads = attend(buf)
    ret = lax.all_to_all(heads, "sp", split_axis=0, concat_axis=0, tiled=True)
    gact = gate(pos, hidden_in, own, sib)
    return mix(pos, ret, gact, own, sib)


def solution(mesh):
    tok = P("dp", "sp", None)
    return jax.shard_map(
        shards,
        mesh=mesh,
        in_specs=(tok, tok, tok, tok, tok, P("dp", "sp"), P("sp", "dp")),
        out_specs=tok,
        check_vma=False,
    )
```
